512 devices in a mesh: fs: 64 (over z, y), tp: 8 (over x, core).
Axes of the slice: x: 4, y: 4, z: 16, core: 2. Of those that a mesh axis runs over, the one named last changes fastest.
Arguments:
- tokens: bfloat16 [24576, 2048], P('fs'), may hold values from -6 to 6
- merged: bfloat16 [24576, 2048], P('fs'), may hold values from -6 to 6
- gain_first: float32 [2048], replicated, may hold values from 0.1 to 1.9
- gate_first: bfloat16 [2048, 2816], P('fs', 'tp'), may hold values from -0.125 to 0.125
- up_first: bfloat16 [2048, 2816], P('fs', 'tp'), may hold values from -0.125 to 0.125
- down_first: bfloat16 [2816, 2048], P('tp', 'fs'), may hold values from -0.21875 to 0.21875
- gain_second: float32 [2048], replicated, may hold values from 0.1 to 1.9
- gate_second: bfloat16 [2048, 2816], P('fs', 'tp'), may hold values from -0.125 to 0.125
- up_second: bfloat16 [2048, 2816], P('fs', 'tp'), may hold values from -0.125 to 0.125
- down_second: bfloat16 [2816, 2048], P('tp', 'fs'), may hold values from -0.21875 to 0.21875
Outputs:
- result: bfloat16 [24576, 2048], P('fs')
The draws below stay inside these ranges and needn't reach their ends.
All inputs are finite; a program needn't handle non-finite values.
Results may differ from the reference program's by a relative error of at most 0.01.
Values may be sent and summed in bfloat16 or wider, within the bound.
No kernel may reach another device: no remote copies, remote signals or barrier semaphores. Data moves between devices by JAX's collectives and lax.ppermute only.
A program may use at most 64 MiB of HBM per device.

```python
import jax
import jax.numpy as jnp
from jax import lax

D = 2048
FF = 2816
TOKENS = 24576
N_TP = 8


def level_of(key, dims, shards, least, largest):
    level = 1.0
    for axis_at, parts in shards:
        draws = jax.random.uniform(jax.random.fold_in(jax.random.fold_in(key, 6), axis_at), (parts,), jnp.float32, least / len(shards), largest / len(shards))
        level = level * jnp.repeat(jnp.exp(draws), dims[axis_at] // parts).reshape((-1,) + (1,) * (len(dims) - 1 - axis_at))
    return level


def scatter_about(rng, dims, deviation, most, split=(), held_as=jnp.bfloat16):
    result = jax.random.normal(rng, dims, jnp.float32) * deviation
    if len(split) > 0:
        result = level_of(rng, dims, split, -0.22, 0.18) * result
    return jnp.clip(result, min=-most, max=most).astype(held_as)


def setup_inputs(seed: int = 0) -> dict:
    seeds = jax.random.split(jax.random.key(seed), 11)
    tokens = scatter_about(seeds[0], (TOKENS, D), 1.0, 6.0, ((0, 64),))
    merged = scatter_about(seeds[1], (TOKENS, D), 1.0, 6.0, ((0, 64),))
    gain_first = jnp.clip(1.0 + 0.18 * jax.random.normal(seeds[2], (D,), jnp.float32), 0.1, 1.9)
    gate_first = scatter_about(seeds[3], (D, FF), D ** -0.5, 0.125, ((0, 64), (1, 8)))
    up_first = scatter_about(seeds[4], (D, FF), D ** -0.5, 0.125, ((0, 64), (1, 8)))
    down_first = scatter_about(seeds[5], (FF, D), (FF // 4) ** -0.5, 0.21875, ((0, 8), (1, 64)))
    gain_second = jnp.clip(1.0 + 0.18 * jax.random.normal(seeds[6], (D,), jnp.float32), 0.1, 1.9)
    gate_second = scatter_about(seeds[7], (D, FF), D ** -0.5, 0.125, ((0, 64), (1, 8)))
    up_second = scatter_about(seeds[8], (D, FF), D ** -0.5, 0.125, ((0, 64), (1, 8)))
    down_second = scatter_about(seeds[9], (FF, D), (FF // 4) ** -0.5, 0.21875, ((0, 8), (1, 64)))
    return {"tokens": tokens, "merged": merged, "gain_first": gain_first, "gate_first": gate_first, "up_first": up_first, "down_first": down_first, "gain_second": gain_second, "gate_second": gate_second, "up_second": up_second, "down_second": down_second}


EPS = 1e-06

def norm_rows(values, gain):
    scale = lax.rsqrt(lax.optimization_barrier(jnp.mean(values * values, axis=-1, keepdims=True)) + EPS)
    return values * scale * gain.astype(jnp.float32)

def half_step(normed, gate_weight, up_weight, down_weight):
    gate = jnp.dot(normed, gate_weight, preferred_element_type=jnp.float32)
    up = jnp.dot(normed, up_weight, preferred_element_type=jnp.float32)
    hidden = (jax.nn.silu(gate) * up).astype(jnp.bfloat16)
    width = FF // N_TP

    def add_block(index, total):
        start = (index * width).astype(jnp.int32)
        cols = lax.dynamic_slice_in_dim(hidden, start, width, 1)
        rows = lax.dynamic_slice_in_dim(down_weight, start, width, 0)
        part = jnp.dot(cols, rows, preferred_element_type=jnp.float32).astype(jnp.bfloat16)
        part = lax.optimization_barrier(part)
        return total + part.astype(jnp.float32)
    empty = jnp.zeros((normed.shape[0], down_weight.shape[1]), jnp.float32)
    return lax.fori_loop(0, N_TP, add_block, empty)

def reference(tokens, merged, gain_first, gate_first, up_first, down_first, gain_second, gate_second, up_second, down_second):
    source = tokens.astype(jnp.float32)
    normed_first = norm_rows(source, gain_first).astype(jnp.bfloat16)
    down_a = half_step(normed_first, gate_first, up_first, down_first)
    middle = source + merged.astype(jnp.float32) + 0.5 * down_a
    normed_second = norm_rows(middle, gain_second).astype(jnp.bfloat16)
    down_b = half_step(normed_second, gate_second, up_second, down_second)
    return (middle + 0.5 * down_b).astype(jnp.bfloat16)
```

```python
import jax
import jax.numpy as jnp
from jax import lax
from jax.sharding import Mesh
from jax.sharding import PartitionSpec as P

FS = ("z", "y")
TP = ("x", "c")
EPS = 1e-06
NZ, NY, NX, NC = 16, 4, 4, 2

W_SCALE = 2.0**18
A_SCALE = 2.0**8


def norm_rows(values, gain):
    scale = lax.rsqrt(jnp.mean(values * values, axis=-1, keepdims=True) + EPS)
    return values * scale * gain


def swap_cores(x):
    return lax.ppermute(x, "c", [(0, 1), (1, 0)])


def half_coded(w):
    return (w.astype(jnp.float32) * W_SCALE).astype(jnp.float16)


def plain(w):
    turned = w.transpose(1, 0, 2, 3).reshape(-1, w.shape[-1])
    return (turned.astype(jnp.float32) * (1.0 / W_SCALE)).astype(jnp.bfloat16)


def gather_weights(mats):
    own = jnp.stack([half_coded(m) for m in mats])
    along_z = lax.all_gather(own, "z", axis=0)
    return lax.all_gather(along_z, "y", axis=0)


def folded(normed, gate_w, up_w):
    gate = jnp.dot(normed, gate_w, preferred_element_type=jnp.float32)
    up = jnp.dot(normed, up_w, preferred_element_type=jnp.float32)
    return (jax.nn.silu(gate) * up).astype(jnp.bfloat16)


def down_dot(hidden, down_t):
    return lax.dot_general(hidden, down_t, (((1,), (1,)), ((), ())), preferred_element_type=jnp.float32)


def summed_at_owner(hidden, down_t, share):
    core = lax.axis_index("c")
    parts = hidden.reshape(NX, NC, share, hidden.shape[-1])
    other = lax.dynamic_index_in_dim(parts, 1 - core, 1, keepdims=False).reshape(NX * share, -1)
    mine = lax.dynamic_index_in_dim(parts, core, 1, keepdims=False).reshape(NX * share, -1)
    sent = swap_cores(down_dot(other, down_t).astype(jnp.bfloat16))
    chip = (down_dot(mine, down_t) + sent.astype(jnp.float32)).astype(jnp.bfloat16)
    pieces = lax.all_to_all(chip.reshape(NX, share, -1), "x", 0, 0, tiled=True)
    return jnp.sum(pieces.astype(jnp.float32), axis=0)


def shards(tokens, merged, gain_first, gate_first, up_first, down_first, gain_second, gate_second, up_second, down_second):
    rows = tokens.shape[0]
    share = rows // (NX * NC)
    core = lax.axis_index("c")
    offset = (lax.axis_index("x") * NC + core) * share
    mats = (gate_first, up_first, down_first.T, gate_second, up_second, down_second.T)
    whole = gather_weights(mats)
    normed_first = norm_rows(tokens.astype(jnp.float32), gain_first).astype(jnp.bfloat16)
    hidden = folded(normed_first, plain(whole[:, :, 0]), plain(whole[:, :, 1]))
    first_sum = summed_at_owner(hidden, plain(whole[:, :, 2]), share)
    base = lax.dynamic_slice_in_dim(tokens, offset, share, 0).astype(jnp.float32)
    extra = lax.dynamic_slice_in_dim(merged, offset, share, 0).astype(jnp.float32)
    middle = base + extra + 0.5 * first_sum
    normed_share = norm_rows(middle, gain_second).astype(jnp.bfloat16)
    coded = (normed_share.astype(jnp.float32) * A_SCALE).astype(jnp.float16)
    everyone = lax.all_gather(coded, TP, axis=0, tiled=True)
    normed_second = (everyone.astype(jnp.float32) * (1.0 / A_SCALE)).astype(jnp.bfloat16)
    hidden_two = folded(normed_second, plain(whole[:, :, 3]), plain(whole[:, :, 4]))
    second_sum = summed_at_owner(hidden_two, plain(whole[:, :, 5]), share)
    finished = (middle + 0.5 * second_sum).astype(jnp.bfloat16)
    mine = lax.all_gather(finished, "x", axis=0)
    theirs = swap_cores(mine)
    low = jnp.where(core == 0, mine, theirs)
    high = jnp.where(core == 0, theirs, mine)
    return jnp.stack([low, high], axis=1).reshape(rows, -1)


def solution(mesh):
    finer = Mesh(mesh.devices.reshape(NZ, NY, NX, NC), ("z", "y", "x", "c"))
    return jax.shard_map(
        shards,
        mesh=finer,
        in_specs=(P(FS, None), P(FS, None), P(), P(FS, TP), P(FS, TP), P(TP, FS), P(), P(FS, TP), P(FS, TP), P(TP, FS)),
        out_specs=P(FS, None),
        check_vma=False,
    )
```

```python
import jax
import jax.numpy as jnp
from jax import lax
from jax.sharding import Mesh
from jax.sharding import PartitionSpec as P


FS = ("z", "y")
TP = ("x", "c")
EPS = 1e-06
NZ, NY, NX, NC = 16, 4, 4, 2

W_SCALE = 2.0**18
A_SCALE = 2.0**8


def norm_rows(values, gain):
    scale = lax.rsqrt(jnp.mean(values * values, axis=-1, keepdims=True) + EPS)
    return values * scale * gain


def swap_cores(x):
    return lax.ppermute(x, "c", [(0, 1), (1, 0)])


def half_coded(w):
    return (w.astype(jnp.float32) * W_SCALE).astype(jnp.float16)


def plain(w):
    return (w.astype(jnp.float32) * (1.0 / W_SCALE)).astype(jnp.bfloat16)


def shifted(x, axis, by):
    size = lax.axis_size(axis)
    return lax.ppermute(x, axis, [(k, (k + by) % size) for k in range(size)])


def gather_weights(first, second):
    own = jnp.stack([half_coded(m) for m in first])
    along_y = lax.all_gather(own, "y", axis=0)
    both = jnp.concatenate([along_y.reshape(-1, *own.shape[1:]), jnp.stack([half_coded(m) for m in second])])
    whole = lax.all_gather(both, "z", axis=0)
    near = whole[:, : NY * len(first)].reshape(NZ, NY, len(first), *own.shape[1:])
    return [plain(near[:, :, k]).reshape(-1, own.shape[-1]) for k in range(len(first))], plain(whole[:, NY * len(first) :])


def send_over_y(piece):
    low = shifted(piece, "y", 1)
    high = shifted(piece, "y", -1)
    far = shifted(piece, "y", 2)
    return piece, low, far, high


def placed(pieces):
    at = lax.axis_index("y")
    buffer = jnp.zeros((NY, *pieces[0].shape), pieces[0].dtype)
    for back, arrived in enumerate(pieces):
        buffer = lax.dynamic_update_index_in_dim(buffer, arrived, (at + NY - back) % NY, 0)
    return [buffer[:, :, k].transpose(1, 0, 2, 3).reshape(-1, buffer.shape[-1]) for k in range(buffer.shape[2])]


def folded(normed, gate_w, up_w):
    gate = jnp.dot(normed, gate_w, preferred_element_type=jnp.float32)
    up = jnp.dot(normed, up_w, preferred_element_type=jnp.float32)
    return (jax.nn.silu(gate) * up).astype(jnp.bfloat16)


def down_dot(hidden, down_t):
    return lax.dot_general(hidden, down_t, (((1,), (1,)), ((), ())), preferred_element_type=jnp.float32)


def summed_at_owner(hidden, down_t, share):
    core = lax.axis_index("c")
    parts = hidden.reshape(NX, NC, share, hidden.shape[-1])
    other = lax.dynamic_index_in_dim(parts, 1 - core, 1, keepdims=False).reshape(NX * share, -1)
    mine = lax.dynamic_index_in_dim(parts, core, 1, keepdims=False).reshape(NX * share, -1)
    sent = swap_cores(down_dot(other, down_t).astype(jnp.bfloat16))
    chip = (down_dot(mine, down_t) + sent.astype(jnp.float32)).astype(jnp.bfloat16)
    pieces = lax.all_to_all(chip.reshape(NX, share, -1), "x", 0, 0, tiled=True)
    return jnp.sum(pieces.astype(jnp.float32), axis=0)


def body(tokens, merged, gain_first, gate_first, up_first, down_first, gain_second, gate_second, up_second, down_second):
    rows = tokens.shape[0]
    share = rows // (NX * NC)
    core = lax.axis_index("c")
    offset = (lax.axis_index("x") * NC + core) * share
    first, piece = gather_weights((gate_first, up_first, down_first.T), (gate_second, up_second, down_second.T))
    pieces = send_over_y(piece)
    normed_first = norm_rows(tokens.astype(jnp.float32), gain_first).astype(jnp.bfloat16)
    hidden = folded(normed_first, first[0], first[1])
    first_sum = summed_at_owner(hidden, first[2], share)
    base = lax.dynamic_slice_in_dim(tokens, offset, share, 0).astype(jnp.float32)
    extra = lax.dynamic_slice_in_dim(merged, offset, share, 0).astype(jnp.float32)
    middle = base + extra + 0.5 * first_sum
    normed_share = norm_rows(middle, gain_second).astype(jnp.bfloat16)
    coded = (normed_share.astype(jnp.float32) * A_SCALE).astype(jnp.float16)
    everyone = lax.all_gather(coded, TP, axis=0, tiled=True)
    everyone, *pieces = lax.optimization_barrier((everyone, *pieces))
    second = placed(pieces)
    normed_second = (everyone.astype(jnp.float32) * (1.0 / A_SCALE)).astype(jnp.bfloat16)
    hidden_two = folded(normed_second, second[0], second[1])
    second_sum = summed_at_owner(hidden_two, second[2], share)
    finished = (middle + 0.5 * second_sum).astype(jnp.bfloat16)
    mine = lax.all_gather(finished, "x", axis=0)
    theirs = swap_cores(mine)
    low = jnp.where(core == 0, mine, theirs)
    high = jnp.where(core == 0, theirs, mine)
    return jnp.stack([low, high], axis=1).reshape(rows, -1)


def solution(mesh):
    finer = Mesh(mesh.devices.reshape(NZ, NY, NX, NC), ("z", "y", "x", "c"))
    return jax.shard_map(
        body,
        mesh=finer,
        in_specs=(P(FS, None), P(FS, None), P(), P(FS, TP), P(FS, TP), P(TP, FS), P(), P(FS, TP), P(FS, TP), P(TP, FS)),
        out_specs=P(FS, None),
        check_vma=False,
    )
```

```python
import jax
import jax.numpy as jnp
from jax import lax
from jax.sharding import Mesh
from jax.sharding import PartitionSpec as P

FS = ("z", "y")
TP = ("x", "c")
EPS = 1e-06
NZ, NY, NX, NC = 16, 4, 4, 2

W_SCALE = 2.0**18
A_SCALE = 2.0**8


def norm_rows(values, gain):
    scale = lax.rsqrt(jnp.mean(values * values, axis=-1, keepdims=True) + EPS)
    return values * scale * gain


def swap_cores(x):
    return lax.ppermute(x, "c", [(0, 1), (1, 0)])


def half_coded(w):
    return (w.astype(jnp.float32) * W_SCALE).astype(jnp.float16)


def plain(w):
    return (w.astype(jnp.float32) * (1.0 / W_SCALE)).astype(jnp.bfloat16)


def gather_weights(first, second):
    count, rows, width = second.shape
    padded = jnp.pad(second.reshape(count * rows, width), ((0, (NY - 1) * count * rows), (0, 0)))
    padded, first = lax.optimization_barrier((padded, first))
    second_y = lax.all_gather(padded, "y", axis=0, tiled=True)
    first_z = lax.all_gather(first, "z", axis=0)
    second_y, first_z = lax.optimization_barrier((second_y, first_z))
    block = second_y.reshape(NY, -1, width)[:, : count * rows].reshape(NY * count * rows, width)
    block, first_z = lax.optimization_barrier((block, first_z))
    second_whole = lax.all_gather(block, "z", axis=0, tiled=True).reshape(NZ, NY, count, rows, width)
    first_whole = lax.all_gather(first_z, "y", axis=1)
    return [[plain(first_whole[:, :, k]).reshape(-1, width) for k in range(count)], [second_whole[:, :, k].reshape(-1, width) for k in range(count)]]


def folded(normed, gate_w, up_w):
    gate = jnp.dot(normed, gate_w, preferred_element_type=jnp.float32)
    up = jnp.dot(normed, up_w, preferred_element_type=jnp.float32)
    return (jax.nn.silu(gate) * up).astype(jnp.bfloat16)


def down_dot(hidden, down_t):
    return lax.dot_general(hidden, down_t, (((1,), (1,)), ((), ())), preferred_element_type=jnp.float32)


def summed_at_owner(hidden, down_t, share):
    core = lax.axis_index("c")
    parts = hidden.reshape(NX, NC, share, hidden.shape[-1])
    other = lax.dynamic_index_in_dim(parts, 1 - core, 1, keepdims=False).reshape(NX * share, -1)
    mine = lax.dynamic_index_in_dim(parts, core, 1, keepdims=False).reshape(NX * share, -1)
    sent = swap_cores(down_dot(other, down_t).astype(jnp.bfloat16))
    chip = (down_dot(mine, down_t) + sent.astype(jnp.float32)).astype(jnp.bfloat16)
    pieces = lax.all_to_all(chip.reshape(NX, share, -1), "x", 0, 0, tiled=True)
    return jnp.sum(pieces.astype(jnp.float32), axis=0)


def body(tokens, merged, gain_first, gate_first, up_first, down_first, gain_second, gate_second, up_second, down_second):
    rows = tokens.shape[0]
    share = rows // (NX * NC)
    core = lax.axis_index("c")
    offset = (lax.axis_index("x") * NC + core) * share
    own_first = jnp.stack([half_coded(w) for w in (gate_first, up_first, down_first.T)])
    first, second = gather_weights(own_first, jnp.stack((gate_second, up_second, down_second.T)))
    normed_first = norm_rows(tokens.astype(jnp.float32), gain_first).astype(jnp.bfloat16)
    hidden = folded(normed_first, first[0], first[1])
    first_sum = summed_at_owner(hidden, first[2], share)
    base = lax.dynamic_slice_in_dim(tokens, offset, share, 0).astype(jnp.float32)
    extra = lax.dynamic_slice_in_dim(merged, offset, share, 0).astype(jnp.float32)
    middle = base + extra + 0.5 * first_sum
    normed_share = norm_rows(middle, gain_second).astype(jnp.bfloat16)
    coded = (normed_share.astype(jnp.float32) * A_SCALE).astype(jnp.float16)
    everyone = lax.all_gather(coded, TP, axis=0, tiled=True)
    normed_second = (everyone.astype(jnp.float32) * (1.0 / A_SCALE)).astype(jnp.bfloat16)
    hidden_two = folded(normed_second, second[0], second[1])
    second_sum = summed_at_owner(hidden_two, second[2], share)
    finished = (middle + 0.5 * second_sum).astype(jnp.bfloat16)
    mine = lax.all_gather(finished, "x", axis=0)
    theirs = swap_cores(mine)
    low = jnp.where(core == 0, mine, theirs)
    high = jnp.where(core == 0, theirs, mine)
    return jnp.stack([low, high], axis=1).reshape(rows, -1)


def solution(mesh):
    finer = Mesh(mesh.devices.reshape(NZ, NY, NX, NC), ("z", "y", "x", "c"))
    return jax.shard_map(
        body,
        mesh=finer,
        in_specs=(P(FS, None), P(FS, None), P(), P(FS, TP), P(FS, TP), P(TP, FS), P(), P(FS, TP), P(FS, TP), P(TP, FS)),
        out_specs=P(FS, None),
        check_vma=False,
    )
```

```python
import jax
import jax.numpy as jnp
from jax import lax
from jax.sharding import Mesh
from jax.sharding import PartitionSpec as P

FS = ("z", "y")
TP = ("x", "c")
EPS = 1e-06
NZ, NY, NX, NC = 16, 4, 4, 2

W_SCALE = 2.0**18
A_SCALE = 2.0**8


def norm_rows(values, gain):
    scale = lax.rsqrt(jnp.mean(values * values, axis=-1, keepdims=True) + EPS)
    return values * scale * gain


def swap_cores(x):
    return lax.ppermute(x, "c", [(0, 1), (1, 0)])


def side_by_side(mats):
    room = -mats[0].shape[1] % 128
    return jnp.concatenate([jnp.pad(m, ((0, 0), (0, room))) for m in mats], axis=1)


def half_coded(w):
    return (w.astype(jnp.float32) * W_SCALE).astype(jnp.float16)


def plain(w):
    return (w.astype(jnp.float32) * (1.0 / W_SCALE)).astype(jnp.bfloat16)


def gather_weights(first, second):
    rows, width = second.shape
    padded = jnp.pad(second, ((0, (NY - 1) * rows), (0, 0)))
    padded, first = lax.optimization_barrier((padded, first))
    second_y = lax.all_gather(padded, "y", axis=0, tiled=True)
    first_z = lax.all_gather(first, "z", axis=0, tiled=True)
    second_y, first_z = lax.optimization_barrier((second_y, first_z))
    block = second_y.reshape(NY, -1, width)[:, :rows].reshape(NY * rows, width)
    block, first_z = lax.optimization_barrier((block, first_z))
    second_whole = lax.all_gather(block, "z", axis=0, tiled=True)
    first_whole = lax.all_gather(first_z.reshape(NZ, rows, width), "y", axis=1, tiled=True)
    return plain(first_whole.reshape(-1, width)), second_whole


def thirds(whole):
    width = whole.shape[1] // 3
    return [whole[:, k * width : (k + 1) * width] for k in range(3)]


def folded(normed, gate_w, up_w):
    gate = jnp.dot(normed, gate_w, preferred_element_type=jnp.float32)
    up = jnp.dot(normed, up_w, preferred_element_type=jnp.float32)
    return (jax.nn.silu(gate) * up).astype(jnp.bfloat16)


def down_dot(hidden, down_t):
    return lax.dot_general(hidden, down_t, (((1,), (1,)), ((), ())), preferred_element_type=jnp.float32)


def pieces_at_owner(hidden, down_t, share):
    core = lax.axis_index("c")
    parts = hidden.reshape(NX, NC, share, hidden.shape[-1])
    other = lax.dynamic_index_in_dim(parts, 1 - core, 1, keepdims=False).reshape(NX * share, -1)
    mine = lax.dynamic_index_in_dim(parts, core, 1, keepdims=False).reshape(NX * share, -1)
    sent = swap_cores(down_dot(other, down_t).astype(jnp.bfloat16))
    chip = (down_dot(mine, down_t) + sent.astype(jnp.float32)).astype(jnp.bfloat16)
    return lax.all_to_all(chip.reshape(NX, share, -1), "x", 0, 0, tiled=True)


def added(pieces):
    return jnp.sum(pieces.astype(jnp.float32), axis=0)


def body(tokens, merged, gain_first, gate_first, up_first, down_first, gain_second, gate_second, up_second, down_second):
    rows = tokens.shape[0]
    share = rows // (NX * NC)
    core = lax.axis_index("c")
    offset = (lax.axis_index("x") * NC + core) * share
    offset, tokens = lax.optimization_barrier((offset, tokens))
    own_first = half_coded(side_by_side((gate_first, up_first, down_first.T)))
    own_second = side_by_side((gate_second, up_second, down_second.T))
    first, second = (thirds(whole) for whole in gather_weights(own_first, own_second))
    normed_first = norm_rows(tokens.astype(jnp.float32), gain_first).astype(jnp.bfloat16)
    hidden = folded(normed_first, first[0], first[1])
    pieces = pieces_at_owner(hidden, first[2], share)
    pieces, tokens, merged, gain_second, offset = lax.optimization_barrier((pieces, tokens, merged, gain_second, offset))
    first_sum = added(pieces)
    base = lax.dynamic_slice_in_dim(tokens, offset, share, 0).astype(jnp.float32)
    extra = lax.dynamic_slice_in_dim(merged, offset, share, 0).astype(jnp.float32)
    middle = base + extra + 0.5 * first_sum
    normed_share = norm_rows(middle, gain_second).astype(jnp.bfloat16)
    coded = (normed_share.astype(jnp.float32) * A_SCALE).astype(jnp.float16)
    everyone = lax.all_gather(coded, TP, axis=0, tiled=True)
    normed_second = (everyone.astype(jnp.float32) * (1.0 / A_SCALE)).astype(jnp.bfloat16)
    hidden_two = folded(normed_second, second[0], second[1])
    second_sum = added(pieces_at_owner(hidden_two, second[2], share))
    finished = (middle + 0.5 * second_sum).astype(jnp.bfloat16)
    mine = lax.all_gather(finished, "x", axis=0)
    theirs = swap_cores(mine)
    low = jnp.where(core == 0, mine, theirs)
    high = jnp.where(core == 0, theirs, mine)
    return jnp.stack([low, high], axis=1).reshape(rows, -1)


def solution(mesh):
    finer = Mesh(mesh.devices.reshape(NZ, NY, NX, NC), ("z", "y", "x", "c"))
    return jax.shard_map(
        body,
        mesh=finer,
        in_specs=(P(FS, None), P(FS, None), P(), P(FS, TP), P(FS, TP), P(TP, FS), P(), P(FS, TP), P(FS, TP), P(TP, FS)),
        out_specs=P(FS, None),
        check_vma=False,
    )
```

```python
import jax
import jax.numpy as jnp
from jax import lax
from jax.sharding import Mesh
from jax.sharding import PartitionSpec as P

FS = ("z", "y")
TP = ("x", "c")
EPS = 1e-06
NZ, NY, NX, NC = 16, 4, 4, 2

W_SCALE = 2.0**18
A_SCALE = 2.0**8


def norm_rows(values, gain):
    scale = lax.rsqrt(jnp.mean(values * values, axis=-1, keepdims=True) + EPS)
    return values * scale * gain


def swap_cores(x):
    return lax.ppermute(x, "c", [(0, 1), (1, 0)])


def side_by_side(mats):
    room = -mats[0].shape[1] % 128
    return jnp.concatenate([jnp.pad(m, ((0, 0), (0, room))) for m in mats], axis=1)


def half_coded(w):
    return (w.astype(jnp.float32) * W_SCALE).astype(jnp.float16)


def plain(w):
    return (w.astype(jnp.float32) * (1.0 / W_SCALE)).astype(jnp.bfloat16)


def gather_weights(first, second):
    rows, width = second.shape
    row = lax.broadcasted_iota(jnp.int32, (NY * rows, width), 0)
    spread = jnp.where(row // rows == lax.axis_index("y"), jnp.tile(second, (NY, 1)), jnp.zeros((), second.dtype))
    spread, first = lax.optimization_barrier((spread, first))
    block = lax.psum(spread, "y")
    first_z = lax.all_gather(first, "z", axis=0, tiled=True)
    block, first_z = lax.optimization_barrier((block, first_z))
    second_whole = lax.all_gather(block, "z", axis=0, tiled=True)
    first_whole = lax.all_gather(first_z.reshape(NZ, rows, width), "y", axis=1, tiled=True)
    return plain(first_whole.reshape(-1, width)), second_whole


def thirds(whole):
    width = whole.shape[1] // 3
    return [whole[:, k * width : (k + 1) * width] for k in range(3)]


def folded(normed, gate_w, up_w):
    gate = jnp.dot(normed, gate_w, preferred_element_type=jnp.float32)
    up = jnp.dot(normed, up_w, preferred_element_type=jnp.float32)
    return (jax.nn.silu(gate) * up).astype(jnp.bfloat16)


def down_dot(hidden, down_t):
    return lax.dot_general(hidden, down_t, (((1,), (1,)), ((), ())), preferred_element_type=jnp.float32)


def pieces_at_owner(hidden, down_t, share):
    core = lax.axis_index("c")
    parts = hidden.reshape(NX, NC, share, hidden.shape[-1])
    other = lax.dynamic_index_in_dim(parts, 1 - core, 1, keepdims=False).reshape(NX * share, -1)
    mine = lax.dynamic_index_in_dim(parts, core, 1, keepdims=False).reshape(NX * share, -1)
    sent = swap_cores(down_dot(other, down_t).astype(jnp.bfloat16))
    chip = (down_dot(mine, down_t) + sent.astype(jnp.float32)).astype(jnp.bfloat16)
    return lax.all_to_all(chip.reshape(NX, share, -1), "x", 0, 0, tiled=True)


def added(pieces):
    return jnp.sum(pieces.astype(jnp.float32), axis=0)


def power_of_two(p):
    size = jnp.abs(p)
    out = jnp.ones(p.shape, jnp.float32)
    for bit in range(7):
        factor = jnp.where(p < 0, 2.0 ** -(2**bit), 2.0 ** (2**bit))
        out = jnp.where((size >> bit) & 1 == 1, out * factor, out)
    return out


def spread_rows(finished):
    share, width = finished.shape
    wide = finished.astype(jnp.float32)
    top = jnp.max(jnp.abs(wide), axis=1, keepdims=True)
    power = jnp.floor(jnp.log2(jnp.maximum(top, 2.0**-100)))
    power = jnp.clip(power, -100.0, 127.0)
    coded = wide * power_of_two(13 - power.astype(jnp.int32))
    tail = jnp.broadcast_to(power, (share, 128))
    sent = jnp.concatenate([coded, tail], axis=1).astype(jnp.float16)
    everyone = lax.all_gather(sent, TP, axis=0, tiled=True)
    back = power_of_two(everyone[:, width : width + 1].astype(jnp.float32).astype(jnp.int32) - 13)
    everyone, back = lax.optimization_barrier((everyone, back))
    return (everyone[:, :width].astype(jnp.float32) * back).astype(jnp.bfloat16)


def body(tokens, merged, gain_first, gate_first, up_first, down_first, gain_second, gate_second, up_second, down_second):
    rows = tokens.shape[0]
    share = rows // (NX * NC)
    core = lax.axis_index("c")
    offset = (lax.axis_index("x") * NC + core) * share
    offset, tokens = lax.optimization_barrier((offset, tokens))
    own_first = half_coded(side_by_side((gate_first, up_first, down_first.T)))
    own_second = side_by_side((gate_second, up_second, down_second.T))
    first, second = (thirds(whole) for whole in gather_weights(own_first, own_second))
    normed_first = norm_rows(tokens.astype(jnp.float32), gain_first).astype(jnp.bfloat16)
    hidden = folded(normed_first, first[0], first[1])
    pieces = pieces_at_owner(hidden, first[2], share)
    pieces, tokens, merged, gain_second, offset = lax.optimization_barrier((pieces, tokens, merged, gain_second, offset))
    first_sum = added(pieces)
    base = lax.dynamic_slice_in_dim(tokens, offset, share, 0).astype(jnp.float32)
    extra = lax.dynamic_slice_in_dim(merged, offset, share, 0).astype(jnp.float32)
    middle = base + extra + 0.5 * first_sum
    normed_share = norm_rows(middle, gain_second).astype(jnp.bfloat16)
    coded = (normed_share.astype(jnp.float32) * A_SCALE).astype(jnp.float16)
    everyone = lax.all_gather(coded, TP, axis=0, tiled=True)
    normed_second = (everyone.astype(jnp.float32) * (1.0 / A_SCALE)).astype(jnp.bfloat16)
    hidden_two = folded(normed_second, second[0], second[1])
    second_sum = added(pieces_at_owner(hidden_two, second[2], share))
    finished = (middle + 0.5 * second_sum).astype(jnp.bfloat16)
    return spread_rows(finished)


def solution(mesh):
    finer = Mesh(mesh.devices.reshape(NZ, NY, NX, NC), ("z", "y", "x", "c"))
    return jax.shard_map(
        body,
        mesh=finer,
        in_specs=(P(FS, None), P(FS, None), P(), P(FS, TP), P(FS, TP), P(TP, FS), P(), P(FS, TP), P(FS, TP), P(TP, FS)),
        out_specs=P(FS, None),
        check_vma=False,
    )
```

```python
import jax
import jax.numpy as jnp
from jax import lax
from jax.sharding import Mesh
from jax.experimental import pallas as pl
from jax.experimental.pallas import tpu as pltpu
from jax.sharding import PartitionSpec as P

FS = ("z", "y")
TP = ("x", "c")
EPS = 1e-06
NZ, NY, NX, NC = 16, 4, 4, 2

W_SCALE = 2.0**18
A_SCALE = 2.0**8


def norm_rows(values, gain):
    scale = lax.rsqrt(jnp.mean(values * values, axis=-1, keepdims=True) + EPS)
    return values * scale * gain


def swap_cores(x):
    return lax.ppermute(x, "c", [(0, 1), (1, 0)])


def side_by_side(mats, times=1):
    rows, columns = mats[0].shape
    return jnp.concatenate([jnp.pad(m, ((0, (times - 1) * rows), (0, -columns % 128))) for m in mats], axis=1)


def half_coded(w):
    return (w.astype(jnp.float32) * W_SCALE).astype(jnp.float16)


def plain(w):
    return (w.astype(jnp.float32) * (1.0 / W_SCALE)).astype(jnp.bfloat16)


def first_rows(padded, rows):
    total, width = padded.shape
    step = total // NY

    def kernel(source, target, sems):
        copies = [
            pltpu.make_async_copy(source.at[pl.ds(k * step, rows)], target.at[pl.ds(k * rows, rows)], sems.at[k])
            for k in range(NY)
        ]
        for copy in copies:
            copy.start()
        for copy in copies:
            copy.wait()

    return pl.pallas_call(
        kernel,
        out_shape=jax.ShapeDtypeStruct((NY * rows, width), padded.dtype),
        in_specs=[pl.BlockSpec(memory_space=pltpu.MemorySpace.HBM)],
        out_specs=pl.BlockSpec(memory_space=pltpu.MemorySpace.HBM),
        scratch_shapes=[pltpu.SemaphoreType.DMA((NY,))],
        name="first_rows",
    )(padded)


CHUNKS = 4


def fold_second(normed, whole, core, share):
    tokens, depth = normed.shape
    width = whole.shape[1] // 3
    step = depth // CHUNKS

    def kernel(core_ref, normed_ref, whole_ref, other_ref, mine_ref, weights, gate, up, hidden, sems):
        copies = [
            pltpu.make_async_copy(whole_ref.at[pl.ds(k * step, step)], weights.at[pl.ds(k * step, step)], sems.at[k])
            for k in range(CHUNKS)
        ]
        for copy in copies:
            copy.start()
        for k, copy in enumerate(copies):
            copy.wait()
            rows = normed_ref[:, pl.ds(k * step, step)]
            here = pl.ds(k * step, step)
            more_gate = jnp.dot(rows, weights[here, 0:width], preferred_element_type=jnp.float32)
            more_up = jnp.dot(rows, weights[here, width : 2 * width], preferred_element_type=jnp.float32)
            if k == 0:
                gate[...] = more_gate
                up[...] = more_up
            elif k < CHUNKS - 1:
                gate[...] += more_gate
                up[...] += more_up
            else:
                total = gate[...] + more_gate
                hidden[...] = (total / (1.0 + jnp.exp(-total)) * (up[...] + more_up)).astype(jnp.bfloat16)
        c = core_ref[0]
        for x in range(NX):
            own = pl.multiple_of((2 * x + c) * share, 16)
            far = pl.multiple_of((2 * x + 1 - c) * share, 16)
            mine_ref[pl.ds(x * share, share), :] = hidden[pl.ds(own, share), :]
            other_ref[pl.ds(x * share, share), :] = lax.dot_general(
                hidden[pl.ds(far, share), :], weights[:, 2 * width :], (((1,), (1,)), ((), ())), preferred_element_type=jnp.float32
            ).astype(jnp.bfloat16)

    vmem = pl.BlockSpec(memory_space=pltpu.MemorySpace.VMEM)
    return pl.pallas_call(
        kernel,
        out_shape=(
            jax.ShapeDtypeStruct((tokens // NC, depth), jnp.bfloat16),
            jax.ShapeDtypeStruct((tokens // NC, width), jnp.bfloat16),
        ),
        in_specs=[pl.BlockSpec(memory_space=pltpu.MemorySpace.SMEM), vmem, pl.BlockSpec(memory_space=pltpu.MemorySpace.HBM)],
        out_specs=(vmem, vmem),
        scratch_shapes=[
            pltpu.VMEM((depth, 3 * width), jnp.bfloat16),
            pltpu.VMEM((tokens, width), jnp.float32),
            pltpu.VMEM((tokens, width), jnp.float32),
            pltpu.VMEM((tokens, width), jnp.bfloat16),
            pltpu.SemaphoreType.DMA((CHUNKS,)),
        ],
        cost_estimate=pl.CostEstimate(flops=3 * tokens * depth * width * 2, bytes_accessed=8_000_000, transcendentals=tokens * width),
        compiler_params=pltpu.CompilerParams(vmem_limit_bytes=50000 * 1024),
        name="fold_second",
    )(jnp.reshape(core, (1,)), normed, whole)


def gather_weights(first, second):
    rows, width = first.shape
    second, first = lax.optimization_barrier((second, first))
    second_y = lax.all_gather(second, "y", axis=0, tiled=True)
    first_z = lax.all_gather(first, "z", axis=0, tiled=True)
    second_y, first_z = lax.optimization_barrier((second_y, first_z))
    block = first_rows(second_y, rows)
    block, first_z = lax.optimization_barrier((block, first_z))
    second_whole = lax.all_gather(block, "z", axis=0, tiled=True)
    first_whole = lax.all_gather(first_z.reshape(NZ, rows, width), "y", axis=1, tiled=True)
    return plain(first_whole.reshape(-1, width)), second_whole


def thirds(whole):
    width = whole.shape[1] // 3
    return [whole[:, k * width : (k + 1) * width] for k in range(3)]


def folded(normed, gate_w, up_w):
    gate = jnp.dot(normed, gate_w, preferred_element_type=jnp.float32)
    up = jnp.dot(normed, up_w, preferred_element_type=jnp.float32)
    return (jax.nn.silu(gate) * up).astype(jnp.bfloat16)


def down_dot(hidden, down_t):
    return lax.dot_general(hidden, down_t, (((1,), (1,)), ((), ())), preferred_element_type=jnp.float32)


def split_rows(hidden, share):
    core = lax.axis_index("c")
    parts = hidden.reshape(NX, NC, share, hidden.shape[-1])
    other = lax.dynamic_index_in_dim(parts, 1 - core, 1, keepdims=False).reshape(NX * share, -1)
    mine = lax.dynamic_index_in_dim(parts, core, 1, keepdims=False).reshape(NX * share, -1)
    return other, mine


def pieces_at_owner(other, mine, down_t, share):
    sent = swap_cores(other)
    chip = (down_dot(mine, down_t) + sent.astype(jnp.float32)).astype(jnp.bfloat16)
    return lax.all_to_all(chip.reshape(NX, share, -1), "x", 0, 0, tiled=True)


def added(pieces):
    return jnp.sum(pieces.astype(jnp.float32), axis=0)


def power_of_two(p):
    size = jnp.abs(p)
    out = jnp.ones(p.shape, jnp.float32)
    for bit in range(7):
        factor = jnp.where(p < 0, 2.0 ** -(2**bit), 2.0 ** (2**bit))
        out = jnp.where((size >> bit) & 1 == 1, out * factor, out)
    return out


def spread_rows(finished):
    share, width = finished.shape
    wide = finished.astype(jnp.float32)
    top = jnp.max(jnp.abs(wide), axis=1, keepdims=True)
    power = jnp.floor(jnp.log2(jnp.maximum(top, 2.0**-100)))
    power = jnp.clip(power, -100.0, 127.0)
    coded = wide * power_of_two(13 - power.astype(jnp.int32))
    tail = jnp.broadcast_to(power, (share, 128))
    sent = jnp.concatenate([coded, tail], axis=1).astype(jnp.float16)
    everyone = lax.all_gather(sent, TP, axis=0, tiled=True)
    back = power_of_two(everyone[:, width : width + 1].astype(jnp.float32).astype(jnp.int32) - 13)
    everyone, back = lax.optimization_barrier((everyone, back))
    return (everyone[:, :width].astype(jnp.float32) * back).astype(jnp.bfloat16)


def body(tokens, merged, gain_first, gate_first, up_first, down_first, gain_second, gate_second, up_second, down_second):
    rows = tokens.shape[0]
    share = rows // (NX * NC)
    core = lax.axis_index("c")
    offset = (lax.axis_index("x") * NC + core) * share
    offset, tokens = lax.optimization_barrier((offset, tokens))
    own_first = half_coded(side_by_side((gate_first, up_first, down_first.T)))
    own_second = side_by_side((gate_second, up_second, down_second.T), NY)
    first_whole, second = gather_weights(own_first, own_second)
    first = thirds(first_whole)
    normed_first = norm_rows(tokens.astype(jnp.float32), gain_first).astype(jnp.bfloat16)
    hidden = folded(normed_first, first[0], first[1])
    other, mine = split_rows(hidden, share)
    pieces = pieces_at_owner(down_dot(other, first[2]).astype(jnp.bfloat16), mine, first[2], share)
    pieces, tokens, merged, gain_second, offset = lax.optimization_barrier((pieces, tokens, merged, gain_second, offset))
    first_sum = added(pieces)
    base = lax.dynamic_slice_in_dim(tokens, offset, share, 0).astype(jnp.float32)
    extra = lax.dynamic_slice_in_dim(merged, offset, share, 0).astype(jnp.float32)
    middle = base + extra + 0.5 * first_sum
    normed_share = norm_rows(middle, gain_second).astype(jnp.bfloat16)
    coded = (normed_share.astype(jnp.float32) * A_SCALE).astype(jnp.float16)
    everyone = lax.all_gather(coded, TP, axis=0, tiled=True)
    normed_second = (everyone.astype(jnp.float32) * (1.0 / A_SCALE)).astype(jnp.bfloat16)
    other, mine = fold_second(normed_second, second, core, share)
    second_sum = added(pieces_at_owner(other, mine, thirds(second)[2], share))
    finished = (middle + 0.5 * second_sum).astype(jnp.bfloat16)
    return spread_rows(finished)


def solution(mesh):
    finer = Mesh(mesh.devices.reshape(NZ, NY, NX, NC), ("z", "y", "x", "c"))
    return jax.shard_map(
        body,
        mesh=finer,
        in_specs=(P(FS, None), P(FS, None), P(), P(FS, TP), P(FS, TP), P(TP, FS), P(), P(FS, TP), P(FS, TP), P(TP, FS)),
        out_specs=P(FS, None),
        check_vma=False,
    )
```

```python
import jax
import jax.numpy as jnp
from jax import lax
from jax.sharding import Mesh
from jax.sharding import PartitionSpec as P

FS = ("z", "y")
TP = ("x", "c")
EPS = 1e-06
NZ, NY, NX, NC = 16, 4, 4, 2

W_SCALE = 2.0**18
A_SCALE = 2.0**8


def norm_rows(values, gain):
    scale = lax.rsqrt(jnp.mean(values * values, axis=-1, keepdims=True) + EPS)
    return values * scale * gain


def swap_cores(x):
    return lax.ppermute(x, "c", [(0, 1), (1, 0)])


def side_by_side(mats, times=1):
    rows, columns = mats[0].shape
    return jnp.concatenate([jnp.pad(m, ((0, (times - 1) * rows), (0, -columns % 128))) for m in mats], axis=1)


def half_coded(w):
    return (w.astype(jnp.float32) * W_SCALE).astype(jnp.float16)


def plain(w):
    return (w.astype(jnp.float32) * (1.0 / W_SCALE)).astype(jnp.bfloat16)


def gather_weights(first, second):
    rows, width = first.shape
    second, first = lax.optimization_barrier((second, first))
    second_y = lax.all_gather(second, "y", axis=0, tiled=True)
    first_z = lax.all_gather(first, "z", axis=0, tiled=True)
    second_y, first_z = lax.optimization_barrier((second_y, first_z))
    block = second_y.reshape(NY, -1, width)[:, :rows].reshape(NY * rows, width)
    block, first_z = lax.optimization_barrier((block, first_z))
    second_whole = lax.all_gather(block, "z", axis=0, tiled=True)
    first_whole = lax.all_gather(first_z.reshape(NZ, rows, width), "y", axis=1, tiled=True)
    return first_whole.reshape(-1, width), second_whole


def thirds(whole):
    width = whole.shape[1] // 3
    return [whole[:, k * width : (k + 1) * width] for k in range(3)]


def folded(normed, gate_w, up_w):
    gate = jnp.dot(normed, gate_w, preferred_element_type=jnp.float32)
    up = jnp.dot(normed, up_w, preferred_element_type=jnp.float32)
    return (jax.nn.silu(gate) * up).astype(jnp.bfloat16)


def down_dot(hidden, down_t):
    return lax.dot_general(hidden, down_t, (((1,), (1,)), ((), ())), preferred_element_type=jnp.float32)


def pieces_at_owner(hidden, down_t, share):
    core = lax.axis_index("c")
    parts = hidden.reshape(NX, NC, share, hidden.shape[-1])
    other = lax.dynamic_index_in_dim(parts, 1 - core, 1, keepdims=False).reshape(NX * share, -1)
    mine = lax.dynamic_index_in_dim(parts, core, 1, keepdims=False).reshape(NX * share, -1)
    sent = swap_cores(down_dot(other, down_t).astype(jnp.bfloat16))
    chip = (down_dot(mine, down_t) + sent.astype(jnp.float32)).astype(jnp.bfloat16)
    return lax.all_to_all(chip.reshape(NX, share, -1), "x", 0, 0, tiled=True)


def added(pieces):
    return jnp.sum(pieces.astype(jnp.float32), axis=0)


def power_of_two(p):
    size = jnp.abs(p)
    out = jnp.ones(p.shape, jnp.float32)
    for bit in range(7):
        factor = jnp.where(p < 0, 2.0 ** -(2**bit), 2.0 ** (2**bit))
        out = jnp.where((size >> bit) & 1 == 1, out * factor, out)
    return out


def spread_rows(finished):
    share, width = finished.shape
    wide = finished.astype(jnp.float32)
    top = jnp.max(jnp.abs(wide), axis=1, keepdims=True)
    power = jnp.floor(jnp.log2(jnp.maximum(top, 2.0**-100)))
    power = jnp.clip(power, -100.0, 127.0)
    coded = wide * power_of_two(13 - power.astype(jnp.int32))
    tail = jnp.broadcast_to(power, (share, 128))
    sent = jnp.concatenate([coded, tail], axis=1).astype(jnp.float16)
    everyone = lax.all_gather(sent, TP, axis=0, tiled=True)
    back = power_of_two(everyone[:, width : width + 1].astype(jnp.float32).astype(jnp.int32) - 13)
    everyone, back = lax.optimization_barrier((everyone, back))
    return (everyone[:, :width].astype(jnp.float32) * back).astype(jnp.bfloat16)


def body(tokens, merged, gain_first, gate_first, up_first, down_first, gain_second, gate_second, up_second, down_second):
    rows = tokens.shape[0]
    share = rows // (NX * NC)
    core = lax.axis_index("c")
    offset = (lax.axis_index("x") * NC + core) * share
    offset, tokens = lax.optimization_barrier((offset, tokens))
    own_first = half_coded(side_by_side((gate_first, up_first, down_first.T)))
    own_second = side_by_side((gate_second, up_second, down_second.T), NY)
    first, second = (thirds(whole) for whole in gather_weights(own_first, own_second))
    first = [plain(w) for w in first]
    normed_first = norm_rows(tokens.astype(jnp.float32), gain_first).astype(jnp.bfloat16)
    hidden = folded(normed_first, first[0], first[1])
    pieces = pieces_at_owner(hidden, first[2], share)
    pieces, tokens, merged, gain_second, offset = lax.optimization_barrier((pieces, tokens, merged, gain_second, offset))
    first_sum = added(pieces)
    base = lax.dynamic_slice_in_dim(tokens, offset, share, 0).astype(jnp.float32)
    extra = lax.dynamic_slice_in_dim(merged, offset, share, 0).astype(jnp.float32)
    middle = base + extra + 0.5 * first_sum
    normed_share = norm_rows(middle, gain_second).astype(jnp.bfloat16)
    coded = (normed_share.astype(jnp.float32) * A_SCALE).astype(jnp.float16)
    everyone = lax.all_gather(coded, TP, axis=0, tiled=True)
    normed_second = (everyone.astype(jnp.float32) * (1.0 / A_SCALE)).astype(jnp.bfloat16)
    hidden_two = folded(normed_second, second[0], second[1])
    second_sum = added(pieces_at_owner(hidden_two, second[2], share))
    finished = (middle + 0.5 * second_sum).astype(jnp.bfloat16)
    return spread_rows(finished)


def solution(mesh):
    finer = Mesh(mesh.devices.reshape(NZ, NY, NX, NC), ("z", "y", "x", "c"))
    return jax.shard_map(
        body,
        mesh=finer,
        in_specs=(P(FS, None), P(FS, None), P(), P(FS, TP), P(FS, TP), P(TP, FS), P(), P(FS, TP), P(FS, TP), P(TP, FS)),
        out_specs=P(FS, None),
        check_vma=False,
    )
```

```python
import jax
import jax.numpy as jnp
from jax import lax
from jax.sharding import Mesh
from jax.sharding import PartitionSpec as P

FS = ("z", "y")
TP = ("x", "c")
EPS = 1e-06
NZ, NY, NX, NC = 16, 4, 4, 2

W_SCALE = 2.0**18
A_SCALE = 2.0**8


def norm_rows(values, gain):
    scale = lax.rsqrt(jnp.mean(values * values, axis=-1, keepdims=True) + EPS)
    return values * scale * gain


def swap_cores(x):
    return lax.ppermute(x, "c", [(0, 1), (1, 0)])


def side_by_side(mats, times=1):
    rows, columns = mats[0].shape
    return jnp.concatenate([jnp.pad(m, ((0, (times - 1) * rows), (0, -columns % 128))) for m in mats], axis=1)


def half_coded(w):
    return (w.astype(jnp.float32) * W_SCALE).astype(jnp.float16)


def plain(w):
    return (w.astype(jnp.float32) * (1.0 / W_SCALE)).astype(jnp.bfloat16)


def gather_weights(first, second):
    rows, width = first.shape
    second, first = lax.optimization_barrier((second, first))
    second_y = lax.all_gather(second, "y", axis=0, tiled=True)
    first_z = lax.all_gather(first, "z", axis=0, tiled=True)
    second_y, first_z = lax.optimization_barrier((second_y, first_z))
    block = second_y.reshape(NY, -1, width)[:, :rows].reshape(NY * rows, width)
    block, first_z = lax.optimization_barrier((block, first_z))
    second_whole = lax.all_gather(block, "z", axis=0, tiled=True)
    first_whole = lax.all_gather(first_z.reshape(NZ, rows, width), "y", axis=1, tiled=True)
    return first_whole.reshape(-1, width), second_whole


def thirds(whole):
    width = whole.shape[1] // 3
    return [whole[:, k * width : (k + 1) * width] for k in range(3)]


def folded(normed, gate_w, up_w):
    gate = jnp.dot(normed, gate_w, preferred_element_type=jnp.float32)
    up = jnp.dot(normed, up_w, preferred_element_type=jnp.float32)
    return (jax.nn.silu(gate) * up).astype(jnp.bfloat16)


def down_dot(hidden, down_t):
    return lax.dot_general(hidden, down_t, (((1,), (1,)), ((), ())), preferred_element_type=jnp.float32)


def pieces_at_owner(hidden, down_t, share):
    core = lax.axis_index("c")
    parts = hidden.reshape(NX, NC, share, hidden.shape[-1])
    other = lax.dynamic_index_in_dim(parts, 1 - core, 1, keepdims=False).reshape(NX * share, -1)
    mine = lax.dynamic_index_in_dim(parts, core, 1, keepdims=False).reshape(NX * share, -1)
    sent = swap_cores(down_dot(other, down_t).astype(jnp.bfloat16))
    chip = (down_dot(mine, down_t) + sent.astype(jnp.float32)).astype(jnp.bfloat16)
    return lax.all_to_all(chip.reshape(NX, share, -1), "x", 0, 0, tiled=True)


def added(pieces):
    return jnp.sum(pieces.astype(jnp.float32), axis=0)


def power_of_two(p):
    size = jnp.abs(p)
    out = jnp.ones(p.shape, jnp.float32)
    for bit in range(7):
        factor = jnp.where(p < 0, 2.0 ** -(2**bit), 2.0 ** (2**bit))
        out = jnp.where((size >> bit) & 1 == 1, out * factor, out)
    return out


def spread_rows(finished):
    share, width = finished.shape
    wide = finished.astype(jnp.float32)
    top = jnp.max(jnp.abs(wide), axis=1, keepdims=True)
    power = jnp.floor(jnp.log2(jnp.maximum(top, 2.0**-100)))
    power = jnp.clip(power, -100.0, 127.0)
    coded = wide * power_of_two(13 - power.astype(jnp.int32))
    tail = jnp.broadcast_to(power, (share, 128))
    sent = jnp.concatenate([coded, tail], axis=1).astype(jnp.float16)
    everyone = lax.all_gather(sent, TP, axis=0, tiled=True)
    back = power_of_two(everyone[:, width : width + 1].astype(jnp.float32).astype(jnp.int32) - 13)
    everyone, back = lax.optimization_barrier((everyone, back))
    return (everyone[:, :width].astype(jnp.float32) * back).astype(jnp.bfloat16)


def body(tokens, merged, gain_first, gate_first, up_first, down_first, gain_second, gate_second, up_second, down_second):
    rows = tokens.shape[0]
    share = rows // (NX * NC)
    core = lax.axis_index("c")
    offset = (lax.axis_index("x") * NC + core) * share
    offset, tokens = lax.optimization_barrier((offset, tokens))
    own_first = half_coded(side_by_side((gate_first, up_first, down_first.T)))
    own_second = side_by_side((gate_second, up_second, down_second.T), NY)
    first, second = gather_weights(own_first, own_second)
    first, tokens = lax.optimization_barrier((first, tokens))
    first, second = thirds(first), thirds(second)
    first = [plain(w) for w in first]
    normed_first = norm_rows(tokens.astype(jnp.float32), gain_first).astype(jnp.bfloat16)
    hidden = folded(normed_first, first[0], first[1])
    extra = lax.dynamic_slice_in_dim(merged, offset, share, 0)
    hidden, extra = lax.optimization_barrier((hidden, extra))
    pieces = pieces_at_owner(hidden, first[2], share)
    pieces, tokens, extra, gain_second, offset = lax.optimization_barrier((pieces, tokens, extra, gain_second, offset))
    first_sum = added(pieces)
    base = lax.dynamic_slice_in_dim(tokens, offset, share, 0).astype(jnp.float32)
    extra = extra.astype(jnp.float32)
    middle = base + extra + 0.5 * first_sum
    normed_share = norm_rows(middle, gain_second).astype(jnp.bfloat16)
    coded = (normed_share.astype(jnp.float32) * A_SCALE).astype(jnp.float16)
    everyone = lax.all_gather(coded, TP, axis=0, tiled=True)
    normed_second = (everyone.astype(jnp.float32) * (1.0 / A_SCALE)).astype(jnp.bfloat16)
    hidden_two = folded(normed_second, second[0], second[1])
    second_sum = added(pieces_at_owner(hidden_two, second[2], share))
    finished = (middle + 0.5 * second_sum).astype(jnp.bfloat16)
    return spread_rows(finished)


def solution(mesh):
    finer = Mesh(mesh.devices.reshape(NZ, NY, NX, NC), ("z", "y", "x", "c"))
    return jax.shard_map(
        body,
        mesh=finer,
        in_specs=(P(FS, None), P(FS, None), P(), P(FS, TP), P(FS, TP), P(TP, FS), P(), P(FS, TP), P(FS, TP), P(TP, FS)),
        out_specs=P(FS, None),
        check_vma=False,
    )
```

```python
import jax
import jax.numpy as jnp
from jax import lax
from jax.sharding import Mesh
from jax.sharding import PartitionSpec as P

FS = ("z", "y")
TP = ("x", "c")
EPS = 1e-06
NZ, NY, NX, NC = 16, 4, 4, 2

W_SCALE = 2.0**18
A_SCALE = 2.0**8


def norm_rows(values, gain):
    scale = lax.rsqrt(jnp.mean(values * values, axis=-1, keepdims=True) + EPS)
    return values * scale * gain


def swap_cores(x):
    return lax.ppermute(x, "c", [(0, 1), (1, 0)])


def side_by_side(mats, times=1):
    rows, columns = mats[0].shape
    return jnp.concatenate([jnp.pad(m, ((0, (times - 1) * rows), (0, -columns % 128))) for m in mats], axis=1)


def half_coded(w):
    return (w.astype(jnp.float32) * W_SCALE).astype(jnp.float16)


def plain(w):
    return (w.astype(jnp.float32) * (1.0 / W_SCALE)).astype(jnp.bfloat16)


def gather_weights(first, second):
    rows, width = first.shape
    second, first = lax.optimization_barrier((second, first))
    second_y = lax.all_gather(second, "y", axis=0, tiled=True)
    first_z = lax.all_gather(first, "z", axis=0, tiled=True)
    second_y, first_z = lax.optimization_barrier((second_y, first_z))
    block = second_y.reshape(NY, -1, width)[:, :rows].reshape(NY * rows, width)
    block, first_z = lax.optimization_barrier((block, first_z))
    second_whole = lax.all_gather(block, "z", axis=0, tiled=True)
    first_whole = lax.all_gather(first_z.reshape(NZ, rows, width), "y", axis=1, tiled=True)
    return first_whole.reshape(-1, width), second_whole


def thirds(whole):
    width = whole.shape[1] // 3
    return [whole[:, k * width : (k + 1) * width] for k in range(3)]


def folded(normed, gate_w, up_w):
    gate = jnp.dot(normed, gate_w, preferred_element_type=jnp.float32)
    up = jnp.dot(normed, up_w, preferred_element_type=jnp.float32)
    return (jax.nn.silu(gate) * up).astype(jnp.bfloat16)


def down_dot(hidden, down_t):
    return lax.dot_general(hidden, down_t, (((1,), (1,)), ((), ())), preferred_element_type=jnp.float32)


def pieces_at_owner(hidden, down_t, share):
    core = lax.axis_index("c")
    parts = hidden.reshape(NX, NC, share, hidden.shape[-1])
    other = lax.dynamic_index_in_dim(parts, 1 - core, 1, keepdims=False).reshape(NX * share, -1)
    mine = lax.dynamic_index_in_dim(parts, core, 1, keepdims=False).reshape(NX * share, -1)
    sent = swap_cores(down_dot(other, down_t).astype(jnp.bfloat16))
    chip = (down_dot(mine, down_t) + sent.astype(jnp.float32)).astype(jnp.bfloat16)
    return lax.all_to_all(chip.reshape(NX, share, -1), "x", 0, 0, tiled=True)


def added(pieces):
    return jnp.sum(pieces.astype(jnp.float32), axis=0)


def power_of_two(p):
    size = jnp.abs(p)
    out = jnp.ones(p.shape, jnp.float32)
    for bit in range(7):
        factor = jnp.where(p < 0, 2.0 ** -(2**bit), 2.0 ** (2**bit))
        out = jnp.where((size >> bit) & 1 == 1, out * factor, out)
    return out


def spread_rows(finished):
    share, width = finished.shape
    wide = finished.astype(jnp.float32)
    top = jnp.max(jnp.abs(wide), axis=1, keepdims=True)
    power = jnp.floor(jnp.log2(jnp.maximum(top, 2.0**-100)))
    power = jnp.clip(power, -100.0, 127.0)
    coded = wide * power_of_two(13 - power.astype(jnp.int32))
    tail = jnp.broadcast_to(power, (share, 128))
    sent = jnp.concatenate([coded, tail], axis=1).astype(jnp.float16)
    everyone = lax.all_gather(sent, TP, axis=0, tiled=True)
    back = power_of_two(everyone[:, width : width + 1].astype(jnp.float32).astype(jnp.int32) - 13)
    everyone, back = lax.optimization_barrier((everyone, back))
    return (everyone[:, :width].astype(jnp.float32) * back).astype(jnp.bfloat16)


def body(tokens, merged, gain_first, gate_first, up_first, down_first, gain_second, gate_second, up_second, down_second):
    rows = tokens.shape[0]
    share = rows // (NX * NC)
    core = lax.axis_index("c")
    offset = (lax.axis_index("x") * NC + core) * share
    offset, tokens = lax.optimization_barrier((offset, tokens))
    own_first = half_coded(side_by_side((gate_first, up_first, down_first.T)))
    own_second = side_by_side((gate_second, up_second, down_second.T), NY)
    first, second = (thirds(whole) for whole in gather_weights(own_first, own_second))
    first = [plain(w) for w in first]
    normed_first = norm_rows(tokens.astype(jnp.float32), gain_first).astype(jnp.bfloat16)
    hidden = folded(normed_first, first[0], first[1])
    extra = lax.dynamic_slice_in_dim(merged, offset, share, 0)
    hidden, extra, tokens = lax.optimization_barrier((hidden, extra, tokens))
    base = lax.dynamic_slice_in_dim(tokens, offset, share, 0)
    hidden, base = lax.optimization_barrier((hidden, base))
    pieces = pieces_at_owner(hidden, first[2], share)
    pieces, base, extra, gain_second = lax.optimization_barrier((pieces, base, extra, gain_second))
    first_sum = added(pieces)
    base = base.astype(jnp.float32)
    extra = extra.astype(jnp.float32)
    middle = base + extra + 0.5 * first_sum
    normed_share = norm_rows(middle, gain_second).astype(jnp.bfloat16)
    coded = (normed_share.astype(jnp.float32) * A_SCALE).astype(jnp.float16)
    everyone = lax.all_gather(coded, TP, axis=0, tiled=True)
    normed_second = (everyone.astype(jnp.float32) * (1.0 / A_SCALE)).astype(jnp.bfloat16)
    hidden_two = folded(normed_second, second[0], second[1])
    second_sum = added(pieces_at_owner(hidden_two, second[2], share))
    finished = (middle + 0.5 * second_sum).astype(jnp.bfloat16)
    return spread_rows(finished)


def solution(mesh):
    finer = Mesh(mesh.devices.reshape(NZ, NY, NX, NC), ("z", "y", "x", "c"))
    return jax.shard_map(
        body,
        mesh=finer,
        in_specs=(P(FS, None), P(FS, None), P(), P(FS, TP), P(FS, TP), P(TP, FS), P(), P(FS, TP), P(FS, TP), P(TP, FS)),
        out_specs=P(FS, None),
        check_vma=False,
    )
```

```python
import jax
import jax.numpy as jnp
from jax import lax
from jax.sharding import Mesh
from jax.sharding import PartitionSpec as P

FS = ("z", "y")
TP = ("x", "c")
EPS = 1e-06
NZ, NY, NX, NC = 16, 4, 4, 2

W_SCALE = 2.0**18
A_SCALE = 2.0**8


def norm_rows(values, gain):
    scale = lax.rsqrt(jnp.mean(values * values, axis=-1, keepdims=True) + EPS)
    return values * scale * gain


def swap_cores(x):
    return lax.ppermute(x, "c", [(0, 1), (1, 0)])


def side_by_side(mats, times=1):
    rows, columns = mats[0].shape
    return jnp.concatenate([jnp.pad(m, ((0, (times - 1) * rows), (0, -columns % 128))) for m in mats], axis=1)


def half_coded(w):
    return (w.astype(jnp.float32) * W_SCALE).astype(jnp.float16)


def plain(w):
    return (w.astype(jnp.float32) * (1.0 / W_SCALE)).astype(jnp.bfloat16)


def gather_weights(first, second):
    rows, width = first.shape
    second, first = lax.optimization_barrier((second, first))
    second_y = lax.all_gather(second, "y", axis=0, tiled=True)
    first_z = lax.all_gather(first, "z", axis=0, tiled=True)
    second_y, first_z = lax.optimization_barrier((second_y, first_z))
    block = second_y.reshape(NY, -1, width)[:, :rows].reshape(NY * rows, width)
    block, first_z = lax.optimization_barrier((block, first_z))
    second_whole = lax.all_gather(block, "z", axis=0, tiled=True)
    first_whole = lax.all_gather(first_z.reshape(NZ, rows, width), "y", axis=1, tiled=True)
    return first_whole.reshape(-1, width), second_whole


def thirds(whole):
    width = whole.shape[1] // 3
    return [whole[:, k * width : (k + 1) * width] for k in range(3)]


def folded(normed, gate_w, up_w):
    gate = jnp.dot(normed, gate_w, preferred_element_type=jnp.float32)
    up = jnp.dot(normed, up_w, preferred_element_type=jnp.float32)
    return (jax.nn.silu(gate) * up).astype(jnp.bfloat16)


def down_dot(hidden, down_t):
    return lax.dot_general(hidden, down_t, (((1,), (1,)), ((), ())), preferred_element_type=jnp.float32)


def pieces_at_owner(hidden, down_t, share):
    core = lax.axis_index("c")
    parts = hidden.reshape(NX, NC, share, hidden.shape[-1])
    other = lax.dynamic_index_in_dim(parts, 1 - core, 1, keepdims=False).reshape(NX * share, -1)
    mine = lax.dynamic_index_in_dim(parts, core, 1, keepdims=False).reshape(NX * share, -1)
    sent = swap_cores(down_dot(other, down_t).astype(jnp.bfloat16))
    chip = (down_dot(mine, down_t) + sent.astype(jnp.float32)).astype(jnp.bfloat16)
    return lax.all_to_all(chip.reshape(NX, share, -1), "x", 0, 0, tiled=True)


def added(pieces):
    return jnp.sum(pieces.astype(jnp.float32), axis=0)


def power_of_two(p):
    size = jnp.abs(p)
    out = jnp.ones(p.shape, jnp.float32)
    for bit in range(7):
        factor = jnp.where(p < 0, 2.0 ** -(2**bit), 2.0 ** (2**bit))
        out = jnp.where((size >> bit) & 1 == 1, out * factor, out)
    return out


def spread_rows(finished):
    share, width = finished.shape
    wide = finished.astype(jnp.float32)
    top = jnp.max(jnp.abs(wide), axis=1, keepdims=True)
    power = jnp.floor(jnp.log2(jnp.maximum(top, 2.0**-100)))
    power = jnp.clip(power, -100.0, 127.0)
    coded = wide * power_of_two(13 - power.astype(jnp.int32))
    tail = jnp.broadcast_to(power, (share, 128))
    sent = jnp.concatenate([coded, tail], axis=1).astype(jnp.float16)
    everyone = lax.all_gather(sent, TP, axis=0, tiled=True)
    back = power_of_two(everyone[:, width : width + 1].astype(jnp.float32).astype(jnp.int32) - 13)
    everyone, back = lax.optimization_barrier((everyone, back))
    return (everyone[:, :width].astype(jnp.float32) * back).astype(jnp.bfloat16)


def body(tokens, merged, gain_first, gate_first, up_first, down_first, gain_second, gate_second, up_second, down_second):
    rows = tokens.shape[0]
    share = rows // (NX * NC)
    core = lax.axis_index("c")
    offset = (lax.axis_index("x") * NC + core) * share
    offset, tokens = lax.optimization_barrier((offset, tokens))
    own_first = half_coded(side_by_side((gate_first, up_first, down_first.T)))
    own_second = side_by_side((gate_second, up_second, down_second.T), NY)
    first, second = gather_weights(own_first, own_second)
    first, tokens = lax.optimization_barrier((first, tokens))
    first, second = thirds(first), thirds(second)
    first = [plain(w) for w in first]
    normed_first = norm_rows(tokens.astype(jnp.float32), gain_first).astype(jnp.bfloat16)
    hidden = folded(normed_first, first[0], first[1])
    extra = lax.dynamic_slice_in_dim(merged, offset, share, 0)
    hidden, extra, tokens = lax.optimization_barrier((hidden, extra, tokens))
    base = lax.dynamic_slice_in_dim(tokens, offset, share, 0)
    hidden, base = lax.optimization_barrier((hidden, base))
    pieces = pieces_at_owner(hidden, first[2], share)
    pieces, base, extra, gain_second = lax.optimization_barrier((pieces, base, extra, gain_second))
    first_sum = added(pieces)
    base = base.astype(jnp.float32)
    extra = extra.astype(jnp.float32)
    middle = base + extra + 0.5 * first_sum
    middle = lax.optimization_barrier(middle)
    normed_share = norm_rows(middle, gain_second).astype(jnp.bfloat16)
    coded = (normed_share.astype(jnp.float32) * A_SCALE).astype(jnp.float16)
    everyone = lax.all_gather(coded, TP, axis=0, tiled=True)
    normed_second = (everyone.astype(jnp.float32) * (1.0 / A_SCALE)).astype(jnp.bfloat16)
    hidden_two = folded(normed_second, second[0], second[1])
    second_sum = added(pieces_at_owner(hidden_two, second[2], share))
    finished = (middle + 0.5 * second_sum).astype(jnp.bfloat16)
    return spread_rows(finished)


def solution(mesh):
    finer = Mesh(mesh.devices.reshape(NZ, NY, NX, NC), ("z", "y", "x", "c"))
    return jax.shard_map(
        body,
        mesh=finer,
        in_specs=(P(FS, None), P(FS, None), P(), P(FS, TP), P(FS, TP), P(TP, FS), P(), P(FS, TP), P(FS, TP), P(TP, FS)),
        out_specs=P(FS, None),
        check_vma=False,
    )
```

```python
import jax
import jax.numpy as jnp
from jax import lax
from jax.sharding import Mesh
from jax.sharding import PartitionSpec as P

FS = ("z", "y")
TP = ("x", "c")
EPS = 1e-06
NZ, NY, NX, NC = 16, 4, 4, 2

W_SCALE = 2.0**18
A_SCALE = 2.0**8


def norm_rows(values, gain):
    scale = lax.rsqrt(jnp.mean(values * values, axis=-1, keepdims=True) + EPS)
    return values * scale * gain


def swap_cores(x):
    return lax.ppermute(x, "c", [(0, 1), (1, 0)])


def side_by_side(mats, times=1):
    rows, columns = mats[0].shape
    return jnp.concatenate([jnp.pad(m, ((0, (times - 1) * rows), (0, -columns % 128))) for m in mats], axis=1)


def half_coded(w):
    return (w.astype(jnp.float32) * W_SCALE).astype(jnp.float16)


def plain(w):
    return (w.astype(jnp.float32) * (1.0 / W_SCALE)).astype(jnp.bfloat16)


def gather_weights(first, second):
    rows, width = first.shape
    second, first = lax.optimization_barrier((second, first))
    second_y = lax.all_gather(second, "y", axis=0, tiled=True)
    first_z = lax.all_gather(first, "z", axis=0, tiled=True)
    second_y, first_z = lax.optimization_barrier((second_y, first_z))
    block = second_y.reshape(NY, -1, width)[:, :rows].reshape(NY * rows, width)
    block, first_z = lax.optimization_barrier((block, first_z))
    second_whole = lax.all_gather(block, "z", axis=0, tiled=True)
    first_whole = lax.all_gather(first_z.reshape(NZ, rows, width), "y", axis=1, tiled=True)
    return first_whole.reshape(-1, width), second_whole


def thirds(whole):
    width = whole.shape[1] // 3
    return [whole[:, k * width : (k + 1) * width] for k in range(3)]


def folded(normed, gate_w, up_w):
    gate = jnp.dot(normed, gate_w, preferred_element_type=jnp.float32)
    up = jnp.dot(normed, up_w, preferred_element_type=jnp.float32)
    return (jax.nn.silu(gate) * up).astype(jnp.bfloat16)


def folded_at_once(normed, both_w):
    both = jnp.dot(normed, both_w, preferred_element_type=jnp.float32)
    half = both.shape[1] // 2
    return (jax.nn.silu(both[:, :half]) * both[:, half:]).astype(jnp.bfloat16)


def down_dot(hidden, down_t):
    return lax.dot_general(hidden, down_t, (((1,), (1,)), ((), ())), preferred_element_type=jnp.float32)


def pieces_at_owner(hidden, down_t, share):
    core = lax.axis_index("c")
    parts = hidden.reshape(NX, NC, share, hidden.shape[-1])
    other = lax.dynamic_index_in_dim(parts, 1 - core, 1, keepdims=False).reshape(NX * share, -1)
    mine = lax.dynamic_index_in_dim(parts, core, 1, keepdims=False).reshape(NX * share, -1)
    sent = swap_cores(down_dot(other, down_t).astype(jnp.bfloat16))
    chip = (down_dot(mine, down_t) + sent.astype(jnp.float32)).astype(jnp.bfloat16)
    return lax.all_to_all(chip.reshape(NX, share, -1), "x", 0, 0, tiled=True)


def added(pieces):
    return jnp.sum(pieces.astype(jnp.float32), axis=0)


def power_of_two(p):
    size = jnp.abs(p)
    out = jnp.ones(p.shape, jnp.float32)
    for bit in range(7):
        factor = jnp.where(p < 0, 2.0 ** -(2**bit), 2.0 ** (2**bit))
        out = jnp.where((size >> bit) & 1 == 1, out * factor, out)
    return out


def spread_rows(finished):
    share, width = finished.shape
    wide = finished.astype(jnp.float32)
    top = jnp.max(jnp.abs(wide), axis=1, keepdims=True)
    power = jnp.floor(jnp.log2(jnp.maximum(top, 2.0**-100)))
    power = jnp.clip(power, -100.0, 127.0)
    coded = wide * power_of_two(13 - power.astype(jnp.int32))
    tail = jnp.broadcast_to(power, (share, 128))
    sent = jnp.concatenate([coded, tail], axis=1).astype(jnp.float16)
    everyone = lax.all_gather(sent, TP, axis=0, tiled=True)
    back = power_of_two(everyone[:, width : width + 1].astype(jnp.float32).astype(jnp.int32) - 13)
    everyone, back = lax.optimization_barrier((everyone, back))
    return (everyone[:, :width].astype(jnp.float32) * back).astype(jnp.bfloat16)


def body(tokens, merged, gain_first, gate_first, up_first, down_first, gain_second, gate_second, up_second, down_second):
    rows = tokens.shape[0]
    share = rows // (NX * NC)
    core = lax.axis_index("c")
    offset = (lax.axis_index("x") * NC + core) * share
    offset, tokens = lax.optimization_barrier((offset, tokens))
    own_first = half_coded(side_by_side((gate_first, up_first, down_first.T)))
    own_second = side_by_side((gate_second, up_second, down_second.T), NY)
    first, second_whole = gather_weights(own_first, own_second)
    first, second = thirds(first), thirds(second_whole)
    first = [plain(w) for w in first]
    normed_first = norm_rows(tokens.astype(jnp.float32), gain_first).astype(jnp.bfloat16)
    hidden = folded(normed_first, first[0], first[1])
    pieces = pieces_at_owner(hidden, first[2], share)
    pieces, tokens, merged, gain_second, offset = lax.optimization_barrier((pieces, tokens, merged, gain_second, offset))
    first_sum = added(pieces)
    base = lax.dynamic_slice_in_dim(tokens, offset, share, 0).astype(jnp.float32)
    extra = lax.dynamic_slice_in_dim(merged, offset, share, 0).astype(jnp.float32)
    middle = base + extra + 0.5 * first_sum
    normed_share = norm_rows(middle, gain_second).astype(jnp.bfloat16)
    coded = (normed_share.astype(jnp.float32) * A_SCALE).astype(jnp.float16)
    everyone = lax.all_gather(coded, TP, axis=0, tiled=True)
    normed_second = (everyone.astype(jnp.float32) * (1.0 / A_SCALE)).astype(jnp.bfloat16)
    hidden_two = folded_at_once(normed_second, second_whole[:, : 2 * second[0].shape[1]])
    second_sum = added(pieces_at_owner(hidden_two, second[2], share))
    finished = (middle + 0.5 * second_sum).astype(jnp.bfloat16)
    return spread_rows(finished)


def solution(mesh):
    finer = Mesh(mesh.devices.reshape(NZ, NY, NX, NC), ("z", "y", "x", "c"))
    return jax.shard_map(
        body,
        mesh=finer,
        in_specs=(P(FS, None), P(FS, None), P(), P(FS, TP), P(FS, TP), P(TP, FS), P(), P(FS, TP), P(FS, TP), P(TP, FS)),
        out_specs=P(FS, None),
        check_vma=False,
    )
```

```python
import jax
import jax.numpy as jnp
from jax import lax
from jax.sharding import Mesh
from jax.sharding import PartitionSpec as P

FS = ("z", "y")
TP = ("x", "c")
EPS = 1e-06
NZ, NY, NX, NC = 16, 4, 4, 2

W_SCALE = 2.0**18
A_SCALE = 2.0**8


def norm_rows(values, gain):
    scale = lax.rsqrt(jnp.mean(values * values, axis=-1, keepdims=True) + EPS)
    return values * scale * gain


def swap_cores(x):
    return lax.ppermute(x, "c", [(0, 1), (1, 0)])


def side_by_side(mats, times=1):
    rows, columns = mats[0].shape
    return jnp.concatenate([jnp.pad(m, ((0, (times - 1) * rows), (0, -columns % 128))) for m in mats], axis=1)


def half_coded(w):
    return (w.astype(jnp.float32) * W_SCALE).astype(jnp.float16)


def plain(w):
    return (w.astype(jnp.float32) * (1.0 / W_SCALE)).astype(jnp.bfloat16)


def gather_weights(first, second):
    rows, width = first.shape
    second, first = lax.optimization_barrier((second, first))
    second_y = lax.all_gather(second, "y", axis=0, tiled=True)
    first_z = lax.all_gather(first, "z", axis=0, tiled=True)
    second_y, first_z = lax.optimization_barrier((second_y, first_z))
    block = second_y.reshape(NY, -1, width)[:, :rows].reshape(NY * rows, width)
    block, first_z = lax.optimization_barrier((block, first_z))
    second_whole = lax.all_gather(block, "z", axis=0, tiled=True)
    first_whole = lax.all_gather(first_z.reshape(NZ, rows, width), "y", axis=1, tiled=True)
    return first_whole.reshape(-1, width), second_whole


def thirds(whole):
    width = whole.shape[1] // 3
    return [whole[:, k * width : (k + 1) * width] for k in range(3)]


def folded_at_once(normed, both_w):
    both = jnp.dot(normed, both_w, preferred_element_type=jnp.float32)
    half = both.shape[1] // 2
    return (jax.nn.silu(both[:, :half]) * both[:, half:]).astype(jnp.bfloat16)


def down_dot(hidden, down_t):
    return lax.dot_general(hidden, down_t, (((1,), (1,)), ((), ())), preferred_element_type=jnp.float32)


def pieces_at_owner(hidden, down_t, share):
    core = lax.axis_index("c")
    parts = hidden.reshape(NX, NC, share, hidden.shape[-1])
    other = lax.dynamic_index_in_dim(parts, 1 - core, 1, keepdims=False).reshape(NX * share, -1)
    mine = lax.dynamic_index_in_dim(parts, core, 1, keepdims=False).reshape(NX * share, -1)
    sent = swap_cores(down_dot(other, down_t).astype(jnp.bfloat16))
    chip = (down_dot(mine, down_t) + sent.astype(jnp.float32)).astype(jnp.bfloat16)
    return lax.all_to_all(chip.reshape(NX, share, -1), "x", 0, 0, tiled=True)


def added(pieces):
    return jnp.sum(pieces.astype(jnp.float32), axis=0)


def power_of_two(p):
    size = jnp.abs(p)
    out = jnp.ones(p.shape, jnp.float32)
    for bit in range(7):
        factor = jnp.where(p < 0, 2.0 ** -(2**bit), 2.0 ** (2**bit))
        out = jnp.where((size >> bit) & 1 == 1, out * factor, out)
    return out


def spread_rows(finished):
    share, width = finished.shape
    wide = finished.astype(jnp.float32)
    top = jnp.max(jnp.abs(wide), axis=1, keepdims=True)
    power = jnp.floor(jnp.log2(jnp.maximum(top, 2.0**-100)))
    power = jnp.clip(power, -100.0, 127.0)
    coded = wide * power_of_two(13 - power.astype(jnp.int32))
    tail = jnp.broadcast_to(power, (share, 128))
    sent = jnp.concatenate([coded, tail], axis=1).astype(jnp.float16)
    everyone = lax.all_gather(sent, TP, axis=0, tiled=True)
    back = power_of_two(everyone[:, width : width + 1].astype(jnp.float32).astype(jnp.int32) - 13)
    everyone, back = lax.optimization_barrier((everyone, back))
    return (everyone[:, :width].astype(jnp.float32) * back).astype(jnp.bfloat16)


def body(tokens, merged, gain_first, gate_first, up_first, down_first, gain_second, gate_second, up_second, down_second):
    rows = tokens.shape[0]
    share = rows // (NX * NC)
    core = lax.axis_index("c")
    offset = (lax.axis_index("x") * NC + core) * share
    offset, tokens = lax.optimization_barrier((offset, tokens))
    own_first = half_coded(side_by_side((gate_first, up_first, down_first.T)))
    own_second = side_by_side((gate_second, up_second, down_second.T), NY)
    first, second_whole = gather_weights(own_first, own_second)
    first_both = plain(first[:, : 2 * first.shape[1] // 3])
    first_down = plain(thirds(first)[2])
    second = thirds(second_whole)
    normed_first = norm_rows(tokens.astype(jnp.float32), gain_first).astype(jnp.bfloat16)
    hidden = folded_at_once(normed_first, first_both)
    pieces = pieces_at_owner(hidden, first_down, share)
    pieces, tokens, merged, gain_second, offset = lax.optimization_barrier((pieces, tokens, merged, gain_second, offset))
    first_sum = added(pieces)
    base = lax.dynamic_slice_in_dim(tokens, offset, share, 0).astype(jnp.float32)
    extra = lax.dynamic_slice_in_dim(merged, offset, share, 0).astype(jnp.float32)
    middle = base + extra + 0.5 * first_sum
    normed_share = norm_rows(middle, gain_second).astype(jnp.bfloat16)
    coded = (normed_share.astype(jnp.float32) * A_SCALE).astype(jnp.float16)
    everyone = lax.all_gather(coded, TP, axis=0, tiled=True)
    normed_second = (everyone.astype(jnp.float32) * (1.0 / A_SCALE)).astype(jnp.bfloat16)
    hidden_two = folded_at_once(normed_second, second_whole[:, : 2 * second[0].shape[1]])
    second_sum = added(pieces_at_owner(hidden_two, second[2], share))
    finished = (middle + 0.5 * second_sum).astype(jnp.bfloat16)
    return spread_rows(finished)


def solution(mesh):
    finer = Mesh(mesh.devices.reshape(NZ, NY, NX, NC), ("z", "y", "x", "c"))
    return jax.shard_map(
        body,
        mesh=finer,
        in_specs=(P(FS, None), P(FS, None), P(), P(FS, TP), P(FS, TP), P(TP, FS), P(), P(FS, TP), P(FS, TP), P(TP, FS)),
        out_specs=P(FS, None),
        check_vma=False,
    )
```

```python
import jax
import jax.numpy as jnp
from jax import lax
from jax.sharding import Mesh
from jax.sharding import PartitionSpec as P

FS = ("z", "y")
TP = ("x", "c")
EPS = 1e-06
NZ, NY, NX, NC = 16, 4, 4, 2

W_SCALE = 2.0**18
A_SCALE = 2.0**8


def norm_rows(values, gain):
    scale = lax.rsqrt(jnp.mean(values * values, axis=-1, keepdims=True) + EPS)
    return values * scale * gain


def swap_cores(x):
    return lax.ppermute(x, "c", [(0, 1), (1, 0)])


def side_by_side(mats, times=1):
    rows, columns = mats[0].shape
    return jnp.concatenate([jnp.pad(m, ((0, (times - 1) * rows), (0, -columns % 128))) for m in mats], axis=1)


def half_coded(w):
    return (w.astype(jnp.float32) * W_SCALE).astype(jnp.float16)


def plain(w):
    return (w.astype(jnp.float32) * (1.0 / W_SCALE)).astype(jnp.bfloat16)


def gather_weights(first, second):
    rows, width = first.shape
    second, first = lax.optimization_barrier((second, first))
    second_y = lax.all_gather(second, "y", axis=0, tiled=True)
    first_z = lax.all_gather(first, "z", axis=0, tiled=True)
    second_y, first_z = lax.optimization_barrier((second_y, first_z))
    block = second_y.reshape(NY, -1, width)[:, :rows].reshape(NY * rows, width)
    block, first_z = lax.optimization_barrier((block, first_z))
    second_whole = lax.all_gather(block, "z", axis=0, tiled=True)
    first_whole = lax.all_gather(first_z.reshape(NZ, rows, width), "y", axis=1, tiled=True)
    return first_whole.reshape(-1, width), second_whole


def thirds(whole):
    width = whole.shape[1] // 3
    return [whole[:, k * width : (k + 1) * width] for k in range(3)]


def folded(normed, gate_w, up_w):
    gate = jnp.dot(normed, gate_w, preferred_element_type=jnp.float32)
    up = jnp.dot(normed, up_w, preferred_element_type=jnp.float32)
    return (jax.nn.silu(gate) * up).astype(jnp.bfloat16)


def folded_at_once(normed, both_w):
    both = jnp.dot(normed, both_w, preferred_element_type=jnp.float32)
    half = both.shape[1] // 2
    return (jax.nn.silu(both[:, :half]) * both[:, half:]).astype(jnp.bfloat16)


def down_dot(hidden, down_t):
    return lax.dot_general(hidden, down_t, (((1,), (1,)), ((), ())), preferred_element_type=jnp.float32)


def pieces_at_owner(hidden, down_t, share):
    core = lax.axis_index("c")
    parts = hidden.reshape(NX, NC, share, hidden.shape[-1])
    other = lax.dynamic_index_in_dim(parts, 1 - core, 1, keepdims=False).reshape(NX * share, -1)
    mine = lax.dynamic_index_in_dim(parts, core, 1, keepdims=False).reshape(NX * share, -1)
    sent = swap_cores(down_dot(other, down_t).astype(jnp.bfloat16))
    chip = (down_dot(mine, down_t) + sent.astype(jnp.float32)).astype(jnp.bfloat16)
    return lax.all_to_all(chip.reshape(NX, share, -1), "x", 0, 0, tiled=True)


def added(pieces):
    return jnp.sum(pieces.astype(jnp.float32), axis=0)


def power_of_two(p):
    size = jnp.abs(p)
    out = jnp.ones(p.shape, jnp.float32)
    for bit in range(7):
        factor = jnp.where(p < 0, 2.0 ** -(2**bit), 2.0 ** (2**bit))
        out = jnp.where((size >> bit) & 1 == 1, out * factor, out)
    return out


def spread_rows(finished):
    share, width = finished.shape
    wide = finished.astype(jnp.float32)
    top = jnp.max(jnp.abs(wide), axis=1, keepdims=True)
    power = jnp.floor(jnp.log2(jnp.maximum(top, 2.0**-100)))
    power = jnp.clip(power, -100.0, 127.0)
    coded = wide * power_of_two(13 - power.astype(jnp.int32))
    tail = jnp.broadcast_to(power, (share, 128))
    sent = jnp.concatenate([coded, tail], axis=1).astype(jnp.float16)
    everyone = lax.all_gather(sent, TP, axis=0, tiled=True)
    back = power_of_two(everyone[:, width : width + 1].astype(jnp.float32).astype(jnp.int32) - 13)
    everyone, back = lax.optimization_barrier((everyone, back))
    return (everyone[:, :width].astype(jnp.float32) * back).astype(jnp.bfloat16)


def body(tokens, merged, gain_first, gate_first, up_first, down_first, gain_second, gate_second, up_second, down_second):
    rows = tokens.shape[0]
    share = rows // (NX * NC)
    core = lax.axis_index("c")
    offset = (lax.axis_index("x") * NC + core) * share
    offset, tokens = lax.optimization_barrier((offset, tokens))
    own_first = half_coded(side_by_side((gate_first, up_first, down_first.T)))
    own_second = side_by_side((gate_second, up_second, down_second.T), NY)
    first, second = gather_weights(own_first, own_second)
    first, tokens = lax.optimization_barrier((first, tokens))
    second_whole = second
    first, second = thirds(first), thirds(second)
    first = [plain(w) for w in first]
    normed_first = norm_rows(tokens.astype(jnp.float32), gain_first).astype(jnp.bfloat16)
    hidden = folded(normed_first, first[0], first[1])
    extra = lax.dynamic_slice_in_dim(merged, offset, share, 0)
    hidden, extra, tokens = lax.optimization_barrier((hidden, extra, tokens))
    base = lax.dynamic_slice_in_dim(tokens, offset, share, 0)
    hidden, base = lax.optimization_barrier((hidden, base))
    pieces = pieces_at_owner(hidden, first[2], share)
    pieces, base, extra, gain_second = lax.optimization_barrier((pieces, base, extra, gain_second))
    first_sum = added(pieces)
    base = base.astype(jnp.float32)
    extra = extra.astype(jnp.float32)
    middle = base + extra + 0.5 * first_sum
    middle = lax.optimization_barrier(middle)
    normed_share = norm_rows(middle, gain_second).astype(jnp.bfloat16)
    coded = (normed_share.astype(jnp.float32) * A_SCALE).astype(jnp.float16)
    everyone = lax.all_gather(coded, TP, axis=0, tiled=True)
    normed_second = (everyone.astype(jnp.float32) * (1.0 / A_SCALE)).astype(jnp.bfloat16)
    hidden_two = folded_at_once(normed_second, second_whole[:, : 2 * second[0].shape[1]])
    second_sum = added(pieces_at_owner(hidden_two, second[2], share))
    finished = (middle + 0.5 * second_sum).astype(jnp.bfloat16)
    return spread_rows(finished)


def solution(mesh):
    finer = Mesh(mesh.devices.reshape(NZ, NY, NX, NC), ("z", "y", "x", "c"))
    return jax.shard_map(
        body,
        mesh=finer,
        in_specs=(P(FS, None), P(FS, None), P(), P(FS, TP), P(FS, TP), P(TP, FS), P(), P(FS, TP), P(FS, TP), P(TP, FS)),
        out_specs=P(FS, None),
        check_vma=False,
    )
```
